32 devices in a mesh: sp: 16 (over z, y, x), tp: 2 (over core).
Axes of the slice: x: 2, y: 2, z: 4, core: 2. Of those that a mesh axis runs over, the one named last changes fastest.
Arguments:
- residual: bfloat16 [3072, 1024], P('sp', 'tp'), may hold values from -6 to 6
- query_first: bfloat16 [3072, 1024], P('sp', 'tp'), may hold values from -64 to 64
- key_first: bfloat16 [3072, 256], P('sp', 'tp'), may hold values from -20 to 20
- value_first: bfloat16 [3072, 256], P('sp', 'tp'), may hold values from -6 to 6
- documents: int32 [3072], P('sp'), may hold values from 0 to 2, as said below
- bias_first: float32 [16, 513], P('tp'), may hold values from -4 to 4
- out_first: bfloat16 [1024, 1024], P('tp'), may hold values from -0.75 to 0.75
- norm_gain: float32 [1024], replicated, may hold values from 0.1 to 1.9
- query_w: bfloat16 [1024, 1024], P(None, 'tp'), may hold values from -0.1875 to 0.1875
- key_w: bfloat16 [1024, 256], P(None, 'tp'), may hold values from -0.1875 to 0.1875
- value_w: bfloat16 [1024, 256], P(None, 'tp'), may hold values from -0.1875 to 0.1875
- bias_second: float32 [16, 513], P('tp'), may hold values from -4 to 4
- out_second: bfloat16 [1024, 1024], P('tp'), may hold values from -0.75 to 0.75
Outputs:
- layer_two: bfloat16 [3072, 1024], P('sp', 'tp')
The draws below stay inside these ranges and needn't reach their ends.
Inputs may be any that keep to these rules, and one draw needn't show every extreme that they name: Document numbers start at 0, never fall, and rise by one at the first position of each document; there are exactly 3 documents, each of at least 896 positions.
All inputs are finite; a program needn't handle non-finite values.
Results may differ from the reference program's by a relative error of at most 0.017.
Values may be sent and summed in bfloat16 or wider, within the bound.
A program may use at most 64 MiB of HBM per device.

```python
import jax
import jax.numpy as jnp
from jax import lax

D = 1024
HEADS = 16
KV_HEADS = 4
HEAD_SIZE = 64
SEG = 64
PAST = 4
REL_CLIP = 256
TOKENS = 3072
DOC_MIN = 896
N_TP = 2


def paired_draw(key):
    base = jax.random.fold_in(key, 11)
    key_noise, query_noise = jax.random.split(base, 2)
    keys_raw = jnp.clip(jax.random.normal(key_noise, (TOKENS, KV_HEADS, HEAD_SIZE), jnp.float32), -4.0, 4.0)
    queries_raw = jnp.clip(jax.random.normal(query_noise, (TOKENS, KV_HEADS, HEADS // KV_HEADS, HEAD_SIZE), jnp.float32), -4.0, 4.0)
    keys_new = keys_raw
    queries_new = queries_raw
    return (queries_new.reshape(TOKENS, HEADS * HEAD_SIZE), keys_new.reshape(TOKENS, KV_HEADS * HEAD_SIZE))


def draw_query_first(key, part):
    return paired_draw(key)[0].astype(jnp.bfloat16)


def draw_key_first(key, part):
    return paired_draw(key)[1].astype(jnp.bfloat16)


def draw_documents(key, part):
    doc_count = TOKENS // DOC_MIN
    spare_rows = TOKENS - doc_count * DOC_MIN
    base = jax.random.fold_in(key, 23)
    cut_points = jnp.sort(jax.random.randint(base, (doc_count,), 0, spare_rows + 1))
    starts = jnp.arange(doc_count) * DOC_MIN + cut_points
    positions = jnp.arange(TOKENS)
    counted = (starts[None, 1:] <= positions[:, None]).astype(jnp.int32)
    return jnp.sum(counted, axis=1).astype(jnp.int32)


def levels(own_key, dims, shards, least, high):
    def one(dim, parts):
        draws = jax.random.uniform(jax.random.fold_in(jax.random.fold_in(own_key, 6), dim), (parts,), jnp.float32, least / len(shards), high / len(shards))
        return jnp.repeat(jnp.exp(draws), dims[dim] // parts).reshape((-1,) + (1,) * (len(dims) - dim - 1))

    loudness = one(*shards[0])
    for cut in shards[1:]:
        loudness = loudness * one(*cut)
    return loudness


def normal_values(own_key, shape, scale, most, shards=(), kind=jnp.bfloat16):
    drawn = scale * jax.random.normal(own_key, shape, jnp.float32)
    if shards:
        drawn = drawn * levels(own_key, shape, shards, -0.22, 0.18)
    return jnp.clip(drawn, -most, most).astype(kind)


def setup_inputs(seed: int = 0) -> dict:
    streams_of = jax.random.split(jax.random.key(seed), 14)
    residual = normal_values(streams_of[0], (TOKENS, D), 1.0, 6.0, ((0, 16), (1, 2)))
    query_first = draw_query_first(jax.random.fold_in(streams_of[13], 71), 0)
    key_first = draw_key_first(jax.random.fold_in(streams_of[13], 71), 0)
    value_first = normal_values(streams_of[3], (TOKENS, KV_HEADS * HEAD_SIZE), 1.0, 6.0, ((0, 16), (1, 2)))
    documents = draw_documents(jax.random.fold_in(streams_of[13], 71), 0)
    bias_first = normal_values(streams_of[5], (HEADS, 2 * REL_CLIP + 1), 1.0, 4.0, ((0, 2),), jnp.float32)
    out_first = normal_values(streams_of[6], (HEADS * HEAD_SIZE, D), (HEADS * HEAD_SIZE // 16) ** -0.5, 0.75, ((0, 2),))
    norm_gain = jnp.clip(1.0 + 0.18 * jax.random.normal(streams_of[7], (D,), jnp.float32), 0.1, 1.9)
    query_w = normal_values(streams_of[8], (D, HEADS * HEAD_SIZE), D ** -0.5, 0.1875, ((1, 2),))
    key_w = normal_values(streams_of[9], (D, KV_HEADS * HEAD_SIZE), D ** -0.5, 0.1875, ((1, 2),))
    value_w = normal_values(streams_of[10], (D, KV_HEADS * HEAD_SIZE), D ** -0.5, 0.1875, ((1, 2),))
    bias_second = normal_values(streams_of[11], (HEADS, 2 * REL_CLIP + 1), 1.0, 4.0, ((0, 2),), jnp.float32)
    out_second = normal_values(streams_of[12], (HEADS * HEAD_SIZE, D), (HEADS * HEAD_SIZE // 16) ** -0.5, 0.75, ((0, 2),))
    return dict(residual=residual, query_first=query_first, key_first=key_first, value_first=value_first, documents=documents, bias_first=bias_first, out_first=out_first, norm_gain=norm_gain, query_w=query_w, key_w=key_w, value_w=value_w, bias_second=bias_second, out_second=out_second)


eps = 1e-06

def segment_attention(queries, keys, values, documents, bias_table):
    total_rows = queries.shape[0]
    span_rows = PAST * SEG
    band_rows = span_rows + SEG
    group_size = HEADS // KV_HEADS
    keys_pad = jnp.concatenate([jnp.zeros((span_rows, keys.shape[1]), keys.dtype), keys], axis=0)
    values_pad = jnp.concatenate([jnp.zeros((span_rows, values.shape[1]), values.dtype), values], axis=0)
    docs_pad = jnp.concatenate([jnp.full((span_rows,), -1, jnp.int32), documents.astype(jnp.int32)], axis=0)
    query_pos = jnp.arange(SEG, dtype=jnp.int32)[:, None]
    key_pos = jnp.arange(band_rows, dtype=jnp.int32)[None, :]
    relative = jnp.clip(query_pos + span_rows - key_pos, -REL_CLIP, REL_CLIP) + REL_CLIP
    position_bias_grid = jnp.take(bias_table.astype(jnp.float32), relative, axis=1).reshape(KV_HEADS, group_size, SEG, band_rows)
    seg_count = total_rows // SEG

    def one_segment(segment):
        first_row = (segment * SEG).astype(jnp.int32)
        query_tile_rows = lax.dynamic_slice_in_dim(queries, first_row, SEG, 0).astype(jnp.float32).reshape(SEG, KV_HEADS, group_size, HEAD_SIZE)
        key_tile_rows = lax.dynamic_slice_in_dim(keys_pad, first_row, band_rows, 0).astype(jnp.float32).reshape(band_rows, KV_HEADS, HEAD_SIZE)
        value_tile_rows = lax.dynamic_slice_in_dim(values_pad, first_row, band_rows, 0).astype(jnp.float32).reshape(band_rows, KV_HEADS, HEAD_SIZE)
        band_docs = lax.dynamic_slice_in_dim(docs_pad, first_row, band_rows, 0)
        own_docs = lax.dynamic_slice_in_dim(documents.astype(jnp.int32), first_row, SEG, 0)
        logit_scores = jnp.einsum('yixw,ziw->ixyz', query_tile_rows, key_tile_rows) * HEAD_SIZE ** (-0.5) + position_bias_grid
        allowed = band_docs[None, :] == own_docs[:, None]
        logit_scores = jnp.where(allowed[None, None], logit_scores, -jnp.inf)
        largest = lax.optimization_barrier(jnp.max(logit_scores, axis=-1, keepdims=True))
        softmax_weight = jnp.exp(logit_scores - largest)
        softmax_weight = (softmax_weight / lax.optimization_barrier(jnp.sum(softmax_weight, axis=-1, keepdims=True))).astype(jnp.bfloat16)
        blended_output = jnp.einsum('rsvh,hru->vrsu', softmax_weight.astype(jnp.float32), value_tile_rows)
        return blended_output.astype(jnp.bfloat16).reshape(SEG, HEADS * HEAD_SIZE)
    blocks = lax.map(one_segment, jnp.arange(seg_count, dtype=jnp.int32))
    return blocks.reshape(total_rows, HEADS * HEAD_SIZE)

def project_out(mixed, weight):
    share_width = mixed.shape[1] // N_TP
    total_sum = jnp.zeros((mixed.shape[0], weight.shape[1]), jnp.float32)
    for group_index in range(N_TP):
        lower = group_index * share_width
        part_sum = jnp.dot(mixed[:, lower:lower + share_width], weight[lower:lower + share_width], preferred_element_type=jnp.float32)
        rounded = lax.optimization_barrier(part_sum.astype(jnp.bfloat16))
        total_sum = total_sum + rounded.astype(jnp.float32)
    return total_sum

def reference(residual, query_first, key_first, value_first, documents, bias_first, out_first, norm_gain, query_w, key_w, value_w, bias_second, out_second):
    mixed_one = segment_attention(query_first, key_first, value_first, documents, bias_first)
    layer_one = (residual.astype(jnp.float32) + project_out(mixed_one, out_first)).astype(jnp.bfloat16)
    rows_wide = layer_one.astype(jnp.float32)
    scale = lax.rsqrt(lax.optimization_barrier(jnp.mean(rows_wide * rows_wide, axis=1, keepdims=True)) + eps)
    normed = (rows_wide * scale * norm_gain.astype(jnp.float32)).astype(jnp.bfloat16)
    query_two = jnp.dot(normed, query_w, preferred_element_type=jnp.float32).astype(jnp.bfloat16)
    key_two = jnp.dot(normed, key_w, preferred_element_type=jnp.float32).astype(jnp.bfloat16)
    value_two = jnp.dot(normed, value_w, preferred_element_type=jnp.float32).astype(jnp.bfloat16)
    mixed_two = segment_attention(query_two, key_two, value_two, documents, bias_second)
    return (layer_one.astype(jnp.float32) + project_out(mixed_two, out_second)).astype(jnp.bfloat16)
```

```python
import functools

import jax
import jax.numpy as jnp
from jax import lax
from jax.experimental import pallas as pl
from jax.experimental.pallas import tpu as pltpu
from jax.sharding import PartitionSpec as P

HEAD_SIZE = 64
SEG = 64
PAST = 4
REL_CLIP = 256
SPAN = PAST * SEG
BAND = SPAN + SEG
LANES = 128
LOG2E = 1.4426950408889634
HIDDEN = -1e30
MESH = pl.DeviceIdType.MESH


eps = 1e-06


def hops_of(tok_rows):
    hops = []
    for distance in range(1, (SPAN + tok_rows - 1) // tok_rows + 1):
        needed = min(tok_rows, SPAN - (distance - 1) * tok_rows)
        hops.append((distance, tok_rows - needed, needed, SPAN - (distance - 1) * tok_rows - needed))
    return hops


def build_bias(table_ref, bias_ref):
    heads_local = table_ref.shape[0]
    group_size = bias_ref.shape[2] // SEG
    lane = lax.broadcasted_iota(jnp.int32, (SEG, LANES), 1)
    low = lane < SEG
    last = REL_CLIP + SPAN

    def tile(head, index):
        if index == 0:
            return jnp.broadcast_to(table_ref[head : head + 1, last : last + 1], (SEG, LANES))
        first = last - index * LANES
        return jnp.broadcast_to(table_ref[head : head + 1, first : first + LANES], (SEG, LANES))

    def piece(head, block, base):
        back = block // 2
        if block % 2 == 0:
            source = jnp.where(low, tile(head, back), tile(head, back + 1))
            shift = base
        else:
            source = tile(head, back + 1)
            shift = (base + SEG) % LANES
        return pltpu.roll(source, shift, 1, stride=1, stride_axis=0)

    for head in range(0, heads_local, 2):
        for block in range(PAST + 1):
            pair = jnp.where(low, piece(head, block, 0), piece(head + 1, block, SEG)) * LOG2E
            group, inner = head // group_size, head % group_size
            bias_ref[group, block * SEG : (block + 1) * SEG, inner * SEG : (inner + 2) * SEG] = pair


def attend(query_ref, kv_ref, bias_ref, mask_ref, mixed_ref):
    tok_rows = query_ref.shape[0]
    kv_local = bias_ref.shape[0]
    group_size = bias_ref.shape[2] // SEG
    kv_width = kv_local * HEAD_SIZE
    for segment in range(tok_rows // SEG):
        rows = slice(segment * SEG, (segment + 1) * SEG)
        band = slice(segment * SEG, segment * SEG + BAND)
        mask = mask_ref[segment]
        mask = jnp.concatenate([mask] * (group_size * SEG // LANES), axis=1)
        for group in range(kv_local):
            keys = kv_ref[band, group * HEAD_SIZE : (group + 1) * HEAD_SIZE]
            values = kv_ref[band, kv_width + group * HEAD_SIZE : kv_width + (group + 1) * HEAD_SIZE]
            first = group * group_size
            queries = jnp.concatenate(
                [
                    query_ref[rows, head * HEAD_SIZE : (head + 1) * HEAD_SIZE]
                    for head in range(first, first + group_size)
                ],
                axis=0,
            )
            scores = lax.dot_general(
                keys, queries, (((1,), (1,)), ((), ())), preferred_element_type=jnp.float32
            )
            scores = scores * (HEAD_SIZE ** (-0.5) * LOG2E) + bias_ref[group] + mask
            largest = jnp.max(scores, axis=0, keepdims=True)
            weight = jnp.exp2(scores - largest)
            total = jnp.sum(weight, axis=0, keepdims=True)
            blended = lax.dot_general(
                values,
                weight.astype(jnp.bfloat16),
                (((0,), (0,)), ((), ())),
                preferred_element_type=jnp.float32,
            )
            blended = blended / total
            for pair in range(group_size // 2):
                turned = jnp.transpose(blended[:, pair * LANES : (pair + 1) * LANES])
                both = jnp.concatenate([turned[:SEG], turned[SEG:]], axis=1)
                column = (first + 2 * pair) * HEAD_SIZE
                mixed_ref[rows, column : column + LANES] = both.astype(jnp.bfloat16)


def kernel(
    n_sp,
    residual_ref,
    query_ref,
    key_ref,
    value_ref,
    docs_ref,
    bias_one_ref,
    bias_two_ref,
    gain_ref,
    out_one_hbm,
    query_w_hbm,
    key_w_hbm,
    value_w_hbm,
    out_two_hbm,
    result_ref,
    w_out_one,
    w_query,
    w_kv,
    w_out_two,
    kv_one,
    kv_two,
    docs_prior,
    docs_col,
    mask,
    table_one,
    table_two,
    mixed,
    query_two,
    residual_full,
    part_own,
    part_in,
    layer,
    send_sem,
    recv_sem,
    load_sem,
):
    me = lax.axis_index("sp")
    my_tp = lax.axis_index("tp")
    other = 1 - my_tp
    tok_rows = residual_ref.shape[0]
    kv_width = key_ref.shape[1]
    chunks, _, wide = part_own.shape
    half = chunks // 2
    hops = hops_of(tok_rows)

    barrier = pltpu.get_barrier_semaphore()
    expected = jnp.int32(1)
    for distance, _, _, _ in hops:
        for step, there in ((distance, me + distance < n_sp), (-distance, me >= distance)):
            expected = expected + there.astype(jnp.int32)

            @pl.when(there)
            def _():
                pl.semaphore_signal(
                    barrier, inc=1, device_id={"sp": me + step}, device_id_type=MESH
                )

    pl.semaphore_signal(barrier, inc=1, device_id={"tp": other}, device_id_type=MESH)

    loads = [
        pltpu.make_async_copy(out_one_hbm, w_out_one, load_sem.at[0]),
        pltpu.make_async_copy(key_w_hbm, w_kv.at[:, pl.ds(0, kv_width)], load_sem.at[1]),
        pltpu.make_async_copy(value_w_hbm, w_kv.at[:, pl.ds(kv_width, kv_width)], load_sem.at[2]),
        pltpu.make_async_copy(query_w_hbm, w_query, load_sem.at[3]),
        pltpu.make_async_copy(out_two_hbm, w_out_two, load_sem.at[4]),
    ]
    for load in loads:
        load.start()

    slot = iter(range(send_sem.shape[0]))

    def remote(src, dst, index, target):
        return pltpu.make_async_remote_copy(
            src_ref=src,
            dst_ref=dst,
            send_sem=send_sem.at[index],
            recv_sem=recv_sem.at[index],
            device_id=target,
            device_id_type=MESH,
        )

    pl.semaphore_wait(barrier, expected)

    first_copies = []
    for distance, row, needed, landing in hops:
        target = {"sp": lax.rem(me + distance, n_sp)}
        here, there = pl.ds(row, needed), pl.ds(landing, needed)
        copies = [
            remote(key_ref.at[here], kv_one.at[there, pl.ds(0, kv_width)], next(slot), target),
            remote(value_ref.at[here], kv_one.at[there, pl.ds(kv_width, kv_width)], next(slot), target),
            remote(docs_ref, docs_prior.at[distance - 1], next(slot), target),
        ]
        first_copies.append((distance, copies))

        @pl.when(me + distance < n_sp)
        def _():
            for copy in copies:
                copy.start()

        @pl.when(me < distance)
        def _():
            empty = jnp.zeros((needed, 2 * kv_width), jnp.bfloat16)
            kv_one[landing : landing + needed] = empty
            kv_two[landing : landing + needed] = empty
            docs_prior[distance - 1] = jnp.full((1, tok_rows), -1, jnp.int32)

    residual_copy = remote(residual_ref, residual_full.at[my_tp], next(slot), {"tp": other})
    residual_copy.start()
    residual_full[my_tp] = residual_ref[...]
    kv_one[SPAN:, :kv_width] = key_ref[...]
    kv_one[SPAN:, kv_width:] = value_ref[...]

    build_bias(bias_one_ref, table_one)
    build_bias(bias_two_ref, table_two)

    def start_sent(distance, copies):
        @pl.when(me + distance < n_sp)
        def _():
            for copy in copies:
                copy.start()

    def wait_arrived(distance, copies):
        @pl.when(me >= distance)
        def _():
            for copy in copies:
                copy.wait_recv()

    def wait_sent(distance, copies):
        @pl.when(me + distance < n_sp)
        def _():
            for copy in copies:
                copy.wait_send()

    for distance, copies in first_copies:
        wait_arrived(distance, copies)

    eye = lax.broadcasted_iota(jnp.int32, (SEG, SEG), 0) == lax.broadcasted_iota(
        jnp.int32, (SEG, SEG), 1
    )

    def put_column(docs, place):
        picked = jnp.where(eye, docs.astype(jnp.float32), 0.0)
        docs_col[place : place + SEG] = jnp.broadcast_to(
            jnp.sum(picked, axis=1, keepdims=True), (SEG, LANES)
        )

    for distance, row, needed, landing in hops:
        for block in range(0, needed, SEG):
            put_column(
                docs_prior[distance - 1, :, row + block : row + block + SEG], landing + block
            )
    for block in range(0, tok_rows, SEG):
        put_column(docs_ref[:, block : block + SEG], SPAN + block)
    for segment in range(tok_rows // SEG):
        own = docs_ref[:, segment * SEG : (segment + 1) * SEG].astype(jnp.float32)
        own = jnp.concatenate([own, own], axis=1)
        same = docs_col[segment * SEG : segment * SEG + BAND] == own
        mask[segment] = jnp.where(same, 0.0, HIDDEN)

    attend(query_ref, kv_one, table_one, mask, mixed)

    loads[0].wait()
    part_copies = []
    for chunk in range(chunks):
        part_own[chunk] = jnp.dot(
            mixed[...],
            w_out_one[:, chunk * wide : (chunk + 1) * wide],
            preferred_element_type=jnp.float32,
        ).astype(jnp.bfloat16)
        copy = remote(part_own.at[chunk], part_in.at[chunk], next(slot), {"tp": other})
        copy.start()
        part_copies.append(copy)

    residual_copy.wait_recv()
    squares = jnp.zeros((tok_rows, 1), jnp.float32)
    for chunk in range(chunks):
        part_copies[chunk].wait_recv()
        column = (chunk % half) * wide
        rows = residual_full[chunk // half, :, column : column + wide].astype(jnp.float32)
        rows = rows + (
            part_own[chunk].astype(jnp.float32) + part_in[chunk].astype(jnp.float32)
        )
        rows = rows.astype(jnp.bfloat16)
        layer[chunk] = rows
        rows = rows.astype(jnp.float32)
        squares = squares + jnp.sum(rows * rows, axis=1, keepdims=True)
    scale = lax.rsqrt(squares / (chunks * wide) + eps)
    normed = jnp.concatenate(
        [
            (
                layer[chunk].astype(jnp.float32)
                * scale
                * gain_ref[:, chunk * wide : (chunk + 1) * wide]
            ).astype(jnp.bfloat16)
            for chunk in range(chunks)
        ],
        axis=1,
    )
    loads[1].wait()
    loads[2].wait()
    kv_two[SPAN:] = jnp.dot(normed, w_kv[...], preferred_element_type=jnp.float32).astype(
        jnp.bfloat16
    )
    second_copies = []
    for distance, row, needed, landing in hops:
        target = {"sp": lax.rem(me + distance, n_sp)}
        copies = [
            remote(
                kv_two.at[pl.ds(SPAN + row, needed)],
                kv_two.at[pl.ds(landing, needed)],
                next(slot),
                target,
            )
        ]
        second_copies.append((distance, copies))
        start_sent(distance, copies)
    loads[3].wait()
    query_two[...] = jnp.dot(normed, w_query[...], preferred_element_type=jnp.float32).astype(
        jnp.bfloat16
    )
    for copy in part_copies:
        copy.wait_send()
    for distance, copies in second_copies:
        wait_arrived(distance, copies)

    attend(query_two, kv_two, table_two, mask, mixed)

    loads[4].wait()
    last_copies = []
    for chunk in range(half):
        column = pl.multiple_of((other * half + chunk) * wide, wide)
        part_own[chunk] = jnp.dot(
            mixed[...], w_out_two[:, pl.ds(column, wide)], preferred_element_type=jnp.float32
        ).astype(jnp.bfloat16)
        copy = remote(part_own.at[chunk], part_in.at[chunks + chunk], next(slot), {"tp": other})
        copy.start()
        last_copies.append(copy)
    for chunk in range(half):
        column = pl.multiple_of((my_tp * half + chunk) * wide, wide)
        part_own[half + chunk] = jnp.dot(
            mixed[...], w_out_two[:, pl.ds(column, wide)], preferred_element_type=jnp.float32
        ).astype(jnp.bfloat16)
    for chunk in range(half):
        last_copies[chunk].wait_recv()
        branch = part_own[half + chunk].astype(jnp.float32) + part_in[chunks + chunk].astype(
            jnp.float32
        )
        result_ref[:, chunk * wide : (chunk + 1) * wide] = (
            layer[my_tp * half + chunk].astype(jnp.float32) + branch
        ).astype(jnp.bfloat16)

    residual_copy.wait_send()
    for distance, copies in first_copies + second_copies:
        wait_sent(distance, copies)
    for copy in last_copies:
        copy.wait_send()


def body(
    residual,
    query_first,
    key_first,
    value_first,
    documents,
    bias_first,
    out_first,
    norm_gain,
    query_w,
    key_w,
    value_w,
    bias_second,
    out_second,
):
    n_sp = lax.axis_size("sp")
    tok_rows, width_local = residual.shape
    query_width = query_first.shape[1]
    kv_width = key_first.shape[1]
    kv_local = kv_width // HEAD_SIZE
    group_width = query_width // kv_local
    wide = width_local // 2
    chunks = out_first.shape[1] // wide
    hops = len(hops_of(tok_rows))
    n_sems = 3 * hops + 1 + chunks + hops + chunks // 2
    vmem = pl.BlockSpec(memory_space=pltpu.VMEM)
    hbm = pl.BlockSpec(memory_space=pl.ANY)
    bf16 = jnp.bfloat16
    return pl.pallas_call(
        functools.partial(kernel, n_sp),
        name="two_layers",
        out_shape=jax.ShapeDtypeStruct((tok_rows, width_local), bf16),
        in_specs=[vmem] * 8 + [hbm] * 5,
        out_specs=vmem,
        scratch_shapes=[
            pltpu.VMEM(out_first.shape, bf16),
            pltpu.VMEM(query_w.shape, bf16),
            pltpu.VMEM((key_w.shape[0], 2 * kv_width), bf16),
            pltpu.VMEM(out_second.shape, bf16),
            pltpu.VMEM((SPAN + tok_rows, 2 * kv_width), bf16),
            pltpu.VMEM((SPAN + tok_rows, 2 * kv_width), bf16),
            pltpu.VMEM((hops, 1, tok_rows), jnp.int32),
            pltpu.VMEM((SPAN + tok_rows, LANES), jnp.float32),
            pltpu.VMEM((tok_rows // SEG, BAND, LANES), jnp.float32),
            pltpu.VMEM((kv_local, BAND, group_width), jnp.float32),
            pltpu.VMEM((kv_local, BAND, group_width), jnp.float32),
            pltpu.VMEM((tok_rows, query_width), bf16),
            pltpu.VMEM((tok_rows, query_width), bf16),
            pltpu.VMEM((2, tok_rows, width_local), bf16),
            pltpu.VMEM((chunks, tok_rows, wide), bf16),
            pltpu.VMEM((chunks + chunks // 2, tok_rows, wide), bf16),
            pltpu.VMEM((chunks, tok_rows, wide), bf16),
            pltpu.SemaphoreType.DMA((n_sems,)),
            pltpu.SemaphoreType.DMA((n_sems,)),
            pltpu.SemaphoreType.DMA((5,)),
        ],
        compiler_params=pltpu.CompilerParams(collective_id=0, has_side_effects=True),
    )(
        residual,
        query_first,
        key_first,
        value_first,
        documents.reshape(1, tok_rows),
        bias_first,
        bias_second,
        norm_gain.reshape(1, -1),
        out_first,
        query_w,
        key_w,
        value_w,
        out_second,
    )


def solution(mesh):
    placed = (
        P("sp", "tp"),
        P("sp", "tp"),
        P("sp", "tp"),
        P("sp", "tp"),
        P("sp"),
        P("tp", None),
        P("tp", None),
        P(),
        P(None, "tp"),
        P(None, "tp"),
        P(None, "tp"),
        P("tp", None),
        P("tp", None),
    )
    return jax.shard_map(body, mesh=mesh, in_specs=placed, out_specs=P("sp", "tp"), check_vma=False)
```

```python
import functools

import jax
import jax.numpy as jnp
from jax import lax
from jax.experimental import pallas as pl
from jax.experimental.pallas import tpu as pltpu
from jax.sharding import PartitionSpec as P

HEAD_SIZE = 64
SEG = 64
PAST = 4
REL_CLIP = 256
SPAN = PAST * SEG
BAND = SPAN + SEG
LANES = 128
LOG2E = 1.4426950408889634
HIDDEN = -1e30
MESH = pl.DeviceIdType.MESH


eps = 1e-06


def hops_of(tok_rows):
    return range(1, (SPAN + tok_rows - 1) // tok_rows + 1)


def pieces_of(tok_rows):
    pieces = []
    for distance in hops_of(tok_rows):
        top = SPAN - (distance - 1) * tok_rows
        bottom = max(0, top - tok_rows)
        cuts = [cut for cut in range(SEG, tok_rows, SEG) if bottom < cut < top]
        edges = [bottom] + cuts + [top]
        for low, high in reversed(list(zip(edges[:-1], edges[1:]))):
            pieces.append((distance, tok_rows - (top - low), high - low, low))
    return pieces


def build_bias(table_ref, bias_ref):
    heads_local = table_ref.shape[0]
    group_size = bias_ref.shape[2] // SEG
    lane = lax.broadcasted_iota(jnp.int32, (SEG, LANES), 1)
    low = lane < SEG
    last = REL_CLIP + SPAN

    def tile(head, index):
        if index == 0:
            return jnp.broadcast_to(table_ref[head : head + 1, last : last + 1], (SEG, LANES))
        first = last - index * LANES
        return jnp.broadcast_to(table_ref[head : head + 1, first : first + LANES], (SEG, LANES))

    def piece(head, block, base):
        back = block // 2
        if block % 2 == 0:
            source = jnp.where(low, tile(head, back), tile(head, back + 1))
            shift = base
        else:
            source = tile(head, back + 1)
            shift = (base + SEG) % LANES
        return pltpu.roll(source, shift, 1, stride=1, stride_axis=0)

    for head in range(0, heads_local, 2):
        for block in range(PAST + 1):
            pair = jnp.where(low, piece(head, block, 0), piece(head + 1, block, SEG)) * LOG2E
            group, inner = head // group_size, head % group_size
            bias_ref[group, block * SEG : (block + 1) * SEG, inner * SEG : (inner + 2) * SEG] = pair


def attend(segments, query_ref, kv_ref, bias_ref, mask_ref, mixed_ref):
    kv_local = bias_ref.shape[0]
    group_size = bias_ref.shape[2] // SEG
    kv_width = kv_local * HEAD_SIZE
    for segment in segments:
        rows = slice(segment * SEG, (segment + 1) * SEG)
        band = slice(segment * SEG, segment * SEG + BAND)
        mask = mask_ref[segment]
        mask = jnp.concatenate([mask] * (group_size * SEG // LANES), axis=1)
        for group in range(kv_local):
            keys = kv_ref[band, group * HEAD_SIZE : (group + 1) * HEAD_SIZE]
            values = kv_ref[band, kv_width + group * HEAD_SIZE : kv_width + (group + 1) * HEAD_SIZE]
            first = group * group_size
            queries = jnp.concatenate(
                [
                    query_ref[rows, head * HEAD_SIZE : (head + 1) * HEAD_SIZE]
                    for head in range(first, first + group_size)
                ],
                axis=0,
            )
            scores = lax.dot_general(
                keys, queries, (((1,), (1,)), ((), ())), preferred_element_type=jnp.float32
            )
            scores = scores * (HEAD_SIZE ** (-0.5) * LOG2E) + bias_ref[group] + mask
            largest = jnp.max(scores, axis=0, keepdims=True)
            weight = jnp.exp2(scores - largest)
            total = jnp.sum(weight, axis=0, keepdims=True)
            blended = lax.dot_general(
                values,
                weight.astype(jnp.bfloat16),
                (((0,), (0,)), ((), ())),
                preferred_element_type=jnp.float32,
            )
            blended = blended / total
            for pair in range(group_size // 2):
                turned = jnp.transpose(blended[:, pair * LANES : (pair + 1) * LANES])
                both = jnp.concatenate([turned[:SEG], turned[SEG:]], axis=1)
                column = (first + 2 * pair) * HEAD_SIZE
                mixed_ref[rows, column : column + LANES] = both.astype(jnp.bfloat16)


def kernel(
    n_sp,
    key_ref,
    value_ref,
    docs_ref,
    bias_one_ref,
    bias_two_ref,
    gain_ref,
    residual_hbm,
    query_hbm,
    out_one_hbm,
    query_w_hbm,
    key_w_hbm,
    value_w_hbm,
    out_two_hbm,
    result_ref,
    w_out_one,
    w_query,
    w_kv,
    w_out_two,
    kv_one,
    kv_two,
    docs_prior,
    docs_col,
    mask,
    table_one,
    table_two,
    mixed,
    query_one,
    query_two,
    residual_full,
    part_own,
    part_in,
    last_in,
    layer,
    normed,
    send_sem,
    recv_sem,
    load_sem,
):
    me = lax.axis_index("sp")
    my_tp = lax.axis_index("tp")
    other = 1 - my_tp
    tok_rows, width_local = residual_hbm.shape
    kv_width = key_ref.shape[1]
    segments = tok_rows // SEG
    hops = hops_of(tok_rows)
    pieces = pieces_of(tok_rows)
    halves = part_own.shape[0]
    blocks = [(range(segments - 1, 0, -1), SEG, tok_rows - SEG), (range(1), 0, SEG)]

    barrier = pltpu.get_barrier_semaphore()
    expected = jnp.int32(1)
    for distance in hops:
        for step, there in ((distance, me + distance < n_sp), (-distance, me >= distance)):
            expected = expected + there.astype(jnp.int32)

            @pl.when(there)
            def _():
                pl.semaphore_signal(
                    barrier, inc=1, device_id={"sp": me + step}, device_id_type=MESH
                )

    pl.semaphore_signal(barrier, inc=1, device_id={"tp": other}, device_id_type=MESH)

    loads = [
        pltpu.make_async_copy(query_hbm, query_one, load_sem.at[0]),
        pltpu.make_async_copy(out_one_hbm, w_out_one, load_sem.at[1]),
        pltpu.make_async_copy(residual_hbm, residual_full.at[my_tp], load_sem.at[2]),
        pltpu.make_async_copy(key_w_hbm, w_kv.at[:, pl.ds(0, kv_width)], load_sem.at[3]),
        pltpu.make_async_copy(value_w_hbm, w_kv.at[:, pl.ds(kv_width, kv_width)], load_sem.at[4]),
        pltpu.make_async_copy(query_w_hbm, w_query, load_sem.at[5]),
        pltpu.make_async_copy(out_two_hbm, w_out_two, load_sem.at[6]),
    ]
    for load in loads:
        load.start()

    slot = iter(range(send_sem.shape[0]))

    def remote(src, dst, target):
        index = next(slot)
        return pltpu.make_async_remote_copy(
            src_ref=src,
            dst_ref=dst,
            send_sem=send_sem.at[index],
            recv_sem=recv_sem.at[index],
            device_id=target,
            device_id_type=MESH,
        )

    def ahead(distance):
        return {"sp": lax.rem(me + distance, n_sp)}

    def start_sent(distance, copies):
        @pl.when(me + distance < n_sp)
        def _():
            for copy in copies:
                copy.start()

    def wait_arrived(distance, copies):
        @pl.when(me >= distance)
        def _():
            for copy in copies:
                copy.wait_recv()

    def wait_sent(distance, copies):
        @pl.when(me + distance < n_sp)
        def _():
            for copy in copies:
                copy.wait_send()

    pl.semaphore_wait(barrier, expected)

    docs_copies = []
    for distance in hops:
        copies = [remote(docs_ref, docs_prior.at[distance - 1], ahead(distance))]
        docs_copies.append((distance, copies))
        start_sent(distance, copies)
    first_copies = []
    for distance, row, needed, landing in pieces:
        here, there = pl.ds(row, needed), pl.ds(landing, needed)
        copies = [
            remote(key_ref.at[here], kv_one.at[there, pl.ds(0, kv_width)], ahead(distance)),
            remote(value_ref.at[here], kv_one.at[there, pl.ds(kv_width, kv_width)], ahead(distance)),
        ]
        first_copies.append((distance, copies))
        start_sent(distance, copies)
    residual_copy = remote(residual_hbm, residual_full.at[my_tp], {"tp": other})
    residual_copy.start()

    for distance, _, needed, landing in pieces:

        @pl.when(me < distance)
        def _():
            empty = jnp.zeros((needed, 2 * kv_width), jnp.bfloat16)
            kv_one[landing : landing + needed] = empty
            kv_two[landing : landing + needed] = empty

    for distance in hops:

        @pl.when(me < distance)
        def _():
            docs_prior[distance - 1] = jnp.full((1, tok_rows), -1, jnp.int32)

    kv_one[SPAN:, :kv_width] = key_ref[...]
    kv_one[SPAN:, kv_width:] = value_ref[...]

    build_bias(bias_one_ref, table_one)
    build_bias(bias_two_ref, table_two)

    for distance, copies in docs_copies:
        wait_arrived(distance, copies)

    eye = lax.broadcasted_iota(jnp.int32, (SEG, SEG), 0) == lax.broadcasted_iota(
        jnp.int32, (SEG, SEG), 1
    )

    def put_column(docs, place):
        picked = jnp.where(eye, docs.astype(jnp.float32), 0.0)
        docs_col[place : place + SEG] = jnp.broadcast_to(
            jnp.sum(picked, axis=1, keepdims=True), (SEG, LANES)
        )

    for distance, row, needed, landing in pieces:
        for block in range(0, needed, SEG):
            put_column(
                docs_prior[distance - 1, :, row + block : row + block + SEG], landing + block
            )
    for block in range(0, tok_rows, SEG):
        put_column(docs_ref[:, block : block + SEG], SPAN + block)
    for segment in range(segments):
        own = docs_ref[:, segment * SEG : (segment + 1) * SEG].astype(jnp.float32)
        own = jnp.concatenate([own, own], axis=1)
        same = docs_col[segment * SEG : segment * SEG + BAND] == own
        mask[segment] = jnp.where(same, 0.0, HIDDEN)

    def attend_block(members, waiting, *refs):
        for segment in members:
            for (distance, _, needed, landing), (_, copies) in zip(pieces, waiting):
                reached = landing + needed > segment * SEG
                earlier = landing + needed > (segment + 1) * SEG
                if reached and not (earlier and segment + 1 < segments):
                    wait_arrived(distance, copies)
            attend([segment], *refs)

    loads[0].wait()
    part_copies = []
    for members, start, count in blocks:
        attend_block(members, first_copies, query_one, kv_one, table_one, mask, mixed)
        if start > 0:
            loads[1].wait()
        rows = pl.ds(start, count)
        copies = []
        for half in range(halves):
            part_own[half, start : start + count] = jnp.dot(
                mixed[start : start + count],
                w_out_one[:, half * width_local : (half + 1) * width_local],
                preferred_element_type=jnp.float32,
            ).astype(jnp.bfloat16)
            copy = remote(part_own.at[half, rows], part_in.at[half, rows], {"tp": other})
            copy.start()
            copies.append(copy)
        part_copies.append(copies)

    loads[2].wait()
    residual_copy.wait_recv()
    second_copies = [None] * len(pieces)
    for (_, start, count), copies in zip(blocks, part_copies):
        rows = slice(start, start + count)
        squares = jnp.zeros((count, 1), jnp.float32)
        for half in range(halves):
            copies[half].wait_recv()
            new = residual_full[half, rows].astype(jnp.float32) + (
                part_own[half, rows].astype(jnp.float32) + part_in[half, rows].astype(jnp.float32)
            )
            new = new.astype(jnp.bfloat16)
            layer[half, rows] = new
            new = new.astype(jnp.float32)
            squares = squares + jnp.sum(new * new, axis=1, keepdims=True)
        scale = lax.rsqrt(squares / (halves * width_local) + eps)
        for half in range(halves):
            columns = slice(half * width_local, (half + 1) * width_local)
            normed[rows, columns] = (
                layer[half, rows].astype(jnp.float32) * scale * gain_ref[:, columns]
            ).astype(jnp.bfloat16)
        if start > 0:
            loads[3].wait()
            loads[4].wait()
        kv_two[SPAN + start : SPAN + start + count] = jnp.dot(
            normed[rows], w_kv[...], preferred_element_type=jnp.float32
        ).astype(jnp.bfloat16)
        for index, (distance, row, needed, landing) in enumerate(pieces):
            if start <= row < start + count:
                piece = remote(
                    kv_two.at[pl.ds(SPAN + row, needed)],
                    kv_two.at[pl.ds(landing, needed)],
                    ahead(distance),
                )
                second_copies[index] = (distance, [piece])
                start_sent(distance, [piece])
    loads[5].wait()
    query_two[...] = jnp.dot(normed[...], w_query[...], preferred_element_type=jnp.float32).astype(
        jnp.bfloat16
    )
    for copies in part_copies:
        for copy in copies:
            copy.wait_send()

    loads[6].wait()
    theirs = pl.ds(pl.multiple_of(other * width_local, width_local), width_local)
    ours = pl.ds(pl.multiple_of(my_tp * width_local, width_local), width_local)
    last_copies = []
    for members, start, count in blocks:
        attend_block(members, second_copies, query_two, kv_two, table_two, mask, mixed)
        rows = pl.ds(start, count)
        part_own[0, start : start + count] = jnp.dot(
            mixed[start : start + count], w_out_two[:, theirs], preferred_element_type=jnp.float32
        ).astype(jnp.bfloat16)
        copy = remote(part_own.at[0, rows], last_in.at[rows], {"tp": other})
        copy.start()
        last_copies.append(copy)
    part_own[1] = jnp.dot(
        mixed[...], w_out_two[:, ours], preferred_element_type=jnp.float32
    ).astype(jnp.bfloat16)
    for (_, start, count), copy in zip(blocks, last_copies):
        rows = slice(start, start + count)
        copy.wait_recv()
        branch = part_own[1, rows].astype(jnp.float32) + last_in[rows].astype(jnp.float32)
        result_ref[rows] = (layer[my_tp, rows].astype(jnp.float32) + branch).astype(jnp.bfloat16)

    residual_copy.wait_send()
    for distance, copies in docs_copies + first_copies + second_copies:
        wait_sent(distance, copies)
    for copy in last_copies:
        copy.wait_send()


def body(
    residual,
    query_first,
    key_first,
    value_first,
    documents,
    bias_first,
    out_first,
    norm_gain,
    query_w,
    key_w,
    value_w,
    bias_second,
    out_second,
):
    n_sp = lax.axis_size("sp")
    tok_rows, width_local = residual.shape
    query_width = query_first.shape[1]
    kv_width = key_first.shape[1]
    kv_local = kv_width // HEAD_SIZE
    group_width = query_width // kv_local
    halves = out_first.shape[1] // width_local
    hops = len(hops_of(tok_rows))
    n_sems = hops + 3 * len(pieces_of(tok_rows)) + 1 + 2 * halves + 2
    vmem = pl.BlockSpec(memory_space=pltpu.VMEM)
    hbm = pl.BlockSpec(memory_space=pl.ANY)
    bf16 = jnp.bfloat16
    return pl.pallas_call(
        functools.partial(kernel, n_sp),
        name="two_layers",
        out_shape=pltpu.VMEM((tok_rows, width_local), bf16),
        in_specs=[vmem] * 6 + [hbm] * 7,
        out_specs=vmem,
        scratch_shapes=[
            pltpu.VMEM(out_first.shape, bf16),
            pltpu.VMEM(query_w.shape, bf16),
            pltpu.VMEM((key_w.shape[0], 2 * kv_width), bf16),
            pltpu.VMEM(out_second.shape, bf16),
            pltpu.VMEM((SPAN + tok_rows, 2 * kv_width), bf16),
            pltpu.VMEM((SPAN + tok_rows, 2 * kv_width), bf16),
            pltpu.VMEM((hops, 1, tok_rows), jnp.int32),
            pltpu.VMEM((SPAN + tok_rows, LANES), jnp.float32),
            pltpu.VMEM((tok_rows // SEG, BAND, LANES), jnp.float32),
            pltpu.VMEM((kv_local, BAND, group_width), jnp.float32),
            pltpu.VMEM((kv_local, BAND, group_width), jnp.float32),
            pltpu.VMEM((tok_rows, query_width), bf16),
            pltpu.VMEM((tok_rows, query_width), bf16),
            pltpu.VMEM((tok_rows, query_width), bf16),
            pltpu.VMEM((halves, tok_rows, width_local), bf16),
            pltpu.VMEM((halves, tok_rows, width_local), bf16),
            pltpu.VMEM((halves, tok_rows, width_local), bf16),
            pltpu.VMEM((tok_rows, width_local), bf16),
            pltpu.VMEM((halves, tok_rows, width_local), bf16),
            pltpu.VMEM((tok_rows, halves * width_local), bf16),
            pltpu.SemaphoreType.DMA((n_sems,)),
            pltpu.SemaphoreType.DMA((n_sems,)),
            pltpu.SemaphoreType.DMA((7,)),
        ],
        compiler_params=pltpu.CompilerParams(collective_id=0, has_side_effects=True),
    )(
        key_first,
        value_first,
        documents.reshape(1, tok_rows),
        bias_first,
        bias_second,
        norm_gain.reshape(1, -1),
        residual,
        query_first,
        out_first,
        query_w,
        key_w,
        value_w,
        out_second,
    )


def solution(mesh):
    placed = (
        P("sp", "tp"),
        P("sp", "tp"),
        P("sp", "tp"),
        P("sp", "tp"),
        P("sp"),
        P("tp", None),
        P("tp", None),
        P(),
        P(None, "tp"),
        P(None, "tp"),
        P(None, "tp"),
        P("tp", None),
        P("tp", None),
    )
    return jax.shard_map(body, mesh=mesh, in_specs=placed, out_specs=P("sp", "tp"), check_vma=False)
```
